32 devices in a mesh: sp: 8 (over z, x), tp: 4 (over y, core).
Axes of the slice: x: 2, y: 2, z: 4, core: 2. Of those that a mesh axis runs over, the one named last changes fastest.
Arguments:
- residual: bfloat16 [6144, 2048], P('sp'), may hold values from -6 to 6
- query_matrix: bfloat16 [6144, 1024], P('sp', 'tp'), may hold values from -6 to 6
- key_matrix: bfloat16 [6144, 1024], P('sp', 'tp'), may hold values from -6 to 6
- value_matrix: bfloat16 [6144, 2048], P('sp', 'tp'), may hold values from -6 to 6
- output_gate_logit: bfloat16 [6144, 2048], P('sp', 'tp'), may hold values from -6 to 6
- input_gate_log: float32 [6144, 8], P('sp', 'tp'), may hold values from -4 to 125
- forget_gate_logit: float32 [6144, 8], P('sp', 'tp')
- extra_head_decay: float32 [6144, 8], P('sp', 'tp'), may hold values from -1 to 0
- head_norm_gain: float32 [2048], P('tp'), may hold values from 0.1 to 1.9
- projection: bfloat16 [2048, 2048], P('tp'), may hold values from -5.303301 to 5.303301
- cell_output_gain: float32 [2048], replicated, may hold values from 0.1 to 1.9
- mixer_input_gain: float32 [2048], replicated, may hold values from 0.1 to 1.9
- mixer_gate_weight: bfloat16 [2048, 5120], P('sp', 'tp'), may hold values from -0.125 to 0.125
- mixer_up_weight: bfloat16 [2048, 5120], P('sp', 'tp'), may hold values from -0.125 to 0.125
- mixer_down_weight: bfloat16 [5120, 2048], P('tp', 'sp'), may hold values from -0.078125 to 0.078125
Outputs:
- updated: bfloat16 [6144, 2048], P('sp', 'tp')
The draws below stay inside these ranges and needn't reach their ends.
All inputs are finite; a program needn't handle non-finite values.
Results may differ from the reference program's by a relative error of at most 0.014.
Values may be sent and summed in bfloat16 or wider, within the bound.
No kernel may reach another device: no remote copies, remote signals or barrier semaphores. Data moves between devices by JAX's collectives and lax.ppermute only.
A program may use at most 128 MiB of HBM per device.

```python
import math
import jax
import jax.numpy as jnp
from jax import lax

D = 2048
HEADS = 8
DQK = 128
DV = 256
FF = 5120
TOK_DEV = 768
TOKENS = 6144
M_V = 2048
N_TP = 4


def draw_input_gate_log(key, part):
    values = jnp.clip(jax.random.normal(key, (TOKENS, HEADS), jnp.float32), -4.0, 4.0)
    return values


def draw_forget_gate_logit(key, part):
    slow_limit = 5
    slow = jax.random.randint(jax.random.fold_in(key, 1), (HEADS,), 0, 10) < slow_limit
    quick = jnp.log(jax.random.uniform(jax.random.fold_in(key, 2), (HEADS,), jnp.float32, 30.0, 60.0))
    level = jnp.where(slow, jnp.log(4.0 * TOKENS), quick)
    shifts = jax.random.uniform(jax.random.fold_in(key, 3), (TOKENS // TOK_DEV, HEADS), jnp.float32, -0.7, 0.7)
    shifts = jnp.repeat(shifts, TOK_DEV, axis=0)
    noise = jnp.clip(jax.random.normal(jax.random.fold_in(key, 4), (TOKENS, HEADS), jnp.float32), -4.0, 4.0)
    return level[None, :] + shifts + noise


def draw_extra_head_decay(key, part):
    spots = jax.random.randint(jax.random.fold_in(key, 1), (3, HEADS), 0, TOKENS)
    depth = jnp.log(jax.random.uniform(jax.random.fold_in(key, 2), (3, HEADS), jnp.float32, 0.5, 0.8))
    columns = lax.broadcasted_iota(jnp.int32, (3, HEADS), 1)
    return jnp.zeros((TOKENS, HEADS), jnp.float32).at[spots, columns].set(depth)


def draw_projection(key, part):
    base = jnp.clip(jax.random.normal(key, (M_V, D), jnp.float32), -6.0, 6.0) * M_V ** (-0.5)
    position = lax.broadcasted_iota(jnp.float32, (1, D), 1) / D
    jitter = jnp.exp(jax.random.uniform(jax.random.fold_in(key, 3), (1, D), jnp.float32, -0.35, 0.35))
    return (base * jnp.exp(1.0986 * position) * jitter).astype(jnp.bfloat16)


def level_of(rng, extent, shards, smallest, top_value):
    loudness = 1.0
    for axis_at, blocks in shards:
        steps = jax.random.uniform(jax.random.fold_in(jax.random.fold_in(rng, 6), axis_at), (blocks,), jnp.float32, smallest / len(shards), top_value / len(shards))
        loudness = loudness * jnp.repeat(jnp.exp(steps), extent[axis_at] // blocks).reshape((-1,) + (1,) * (len(extent) - 1 - axis_at))
    return loudness


def centred(stream_key, dims, scale, reach, cuts=(), kind=jnp.bfloat16):
    values = jax.random.normal(stream_key, dims, jnp.float32) * scale
    if len(cuts) > 0:
        values = level_of(stream_key, dims, cuts, -0.22, 0.18) * values
    return jnp.clip(values, min=-reach, max=reach).astype(kind)


def setup_inputs(seed: int = 0) -> dict:
    arg_keys = jax.random.split(jax.random.key(seed), 16)
    return {
        "residual": centred(arg_keys[0], (TOKENS, D), 1.0, 6.0, ((0, 8),)),
        "query_matrix": centred(arg_keys[1], (TOKENS, HEADS * DQK), 1.0, 6.0, ((0, 8), (1, 4))),
        "key_matrix": centred(arg_keys[2], (TOKENS, HEADS * DQK), 1.0, 6.0, ((0, 8), (1, 4))),
        "value_matrix": centred(arg_keys[3], (TOKENS, M_V), 1.0, 6.0, ((0, 8), (1, 4))),
        "output_gate_logit": centred(arg_keys[4], (TOKENS, M_V), 1.0, 6.0, ((0, 8), (1, 4))),
        "input_gate_log": draw_input_gate_log(jax.random.fold_in(arg_keys[15], 71), 0),
        "forget_gate_logit": draw_forget_gate_logit(jax.random.fold_in(arg_keys[15], 71), 0),
        "extra_head_decay": draw_extra_head_decay(jax.random.fold_in(arg_keys[15], 71), 0),
        "head_norm_gain": jnp.clip(1.0 + 0.18 * jax.random.normal(arg_keys[8], (M_V,), jnp.float32), 0.1, 1.9),
        "projection": draw_projection(jax.random.fold_in(arg_keys[15], 71), 0),
        "cell_output_gain": jnp.clip(1.0 + 0.18 * jax.random.normal(arg_keys[10], (D,), jnp.float32), 0.1, 1.9),
        "mixer_input_gain": jnp.clip(1.0 + 0.18 * jax.random.normal(arg_keys[11], (D,), jnp.float32), 0.1, 1.9),
        "mixer_gate_weight": centred(arg_keys[12], (D, FF), D ** -0.5, 0.125, ((0, 8), (1, 4))),
        "mixer_up_weight": centred(arg_keys[13], (D, FF), D ** -0.5, 0.125, ((0, 8), (1, 4))),
        "mixer_down_weight": centred(arg_keys[14], (FF, D), FF ** -0.5, 0.078125, ((0, 4), (1, 8))),
    }


HIGHEST = lax.Precision.HIGHEST
EPSILON = 1e-06

def read_out(query, keyed, valued, in_logs, running_log_total, memory, normalizer, stabilizer):
    length = query.shape[1]
    causal = lax.broadcasted_iota(jnp.int32, (length, length), 0) >= lax.broadcasted_iota(jnp.int32, (length, length), 1)
    spread = running_log_total[:, :, None] - running_log_total[:, None, :] + in_logs[:, None, :]
    spread = jnp.where(causal[None], spread, -jnp.inf)
    carried = running_log_total + stabilizer[:, None]
    running = jnp.maximum(carried, lax.optimization_barrier(jnp.max(spread, axis=-1)))
    scores = jnp.einsum('htd,hsd->hts', query, keyed, precision=HIGHEST) * DQK ** (-0.5)
    weights = jnp.exp(spread - running[:, :, None]) * scores
    weight_low = lax.optimization_barrier(weights.astype(jnp.bfloat16)).astype(jnp.float32)
    scaled = jnp.exp(carried - running)
    scaled_query = query * DQK ** (-0.5)
    numerator = jnp.einsum('hts,hsv->htv', weight_low, valued, precision=HIGHEST)
    numerator = numerator + scaled[:, :, None] * jnp.einsum('hvd,htd->htv', memory, scaled_query, precision=HIGHEST)
    denominator = lax.optimization_barrier(jnp.sum(weights, axis=-1)) + scaled * jnp.einsum('hd,htd->ht', normalizer, scaled_query, precision=HIGHEST)
    return numerator / jnp.maximum(jnp.abs(denominator), jnp.exp(-running))[:, :, None]

def fold_state(keyed, valued, in_logs, running_log_total, memory, normalizer, stabilizer):
    last = running_log_total[:, -1]
    lifted = last[:, None] - running_log_total + in_logs
    new_max = jnp.maximum(last + stabilizer, lax.optimization_barrier(jnp.max(lifted, axis=-1)))
    weights = jnp.exp(lifted - new_max[:, None])
    retained = jnp.exp(last + stabilizer - new_max)
    memory = retained[:, None, None] * memory + jnp.einsum('hsv,hsd->hvd', weights[:, :, None] * valued, keyed, precision=HIGHEST)
    normalizer = retained[:, None] * normalizer + jnp.einsum('hs,hsd->hd', weights, keyed, precision=HIGHEST)
    return (memory, normalizer, new_max)

def block_sum(left, right, parts):
    rows = left.shape[0]
    inner = left.shape[1] // parts
    left_blocks = left.reshape(rows, parts, inner).transpose(1, 0, 2)
    right_blocks = right.reshape(parts, inner, right.shape[1])

    def accumulate(total, pair):
        product = jnp.dot(pair[0], pair[1], preferred_element_type=jnp.float32).astype(jnp.bfloat16)
        return (total + lax.optimization_barrier(product).astype(jnp.float32), None)
    total, unused = lax.scan(accumulate, jnp.zeros((rows, right.shape[1]), jnp.float32), (left_blocks, right_blocks))
    return total

def reference(residual, query_matrix, key_matrix, value_matrix, output_gate_logit, input_gate_log, forget_gate_logit, extra_head_decay, head_norm_gain, projection, cell_output_gain, mixer_input_gain, mixer_gate_weight, mixer_up_weight, mixer_down_weight):
    span = math.gcd(TOKENS, 512)
    count = TOKENS // span

    def arrange(array, width):
        return array.astype(jnp.float32).reshape(count, span, HEADS, width).transpose(0, 2, 1, 3)
    query = arrange(query_matrix, DQK)
    keyed = arrange(key_matrix, DQK)
    valued = arrange(value_matrix, DV)
    in_logs = input_gate_log.reshape(count, span, HEADS).transpose(0, 2, 1)
    forget_log_value = jax.nn.log_sigmoid(forget_gate_logit) + extra_head_decay
    running_log_total = jnp.cumsum(forget_log_value.reshape(count, span, HEADS), axis=1).transpose(0, 2, 1)

    def advance(state, blocks):
        memory, normalizer, stabilizer = state
        query_block, key_block, value_block, gate_block, decay_block = blocks
        cells = read_out(query_block, key_block, value_block, gate_block, decay_block, memory, normalizer, stabilizer)
        return (fold_state(key_block, value_block, gate_block, decay_block, memory, normalizer, stabilizer), cells)
    start = (jnp.zeros((HEADS, DV, DQK), jnp.float32), jnp.zeros((HEADS, DQK), jnp.float32), jnp.zeros((HEADS,), jnp.float32))
    unused, cells = lax.scan(advance, start, (query, keyed, valued, in_logs, running_log_total))
    centered = cells - lax.optimization_barrier(jnp.mean(cells, axis=-1, keepdims=True))
    normed = centered * lax.rsqrt(lax.optimization_barrier(jnp.mean(centered * centered, axis=-1, keepdims=True)) + EPSILON)
    normed = normed * head_norm_gain.reshape(HEADS, DV)[None, :, None, :]
    normed = normed.transpose(0, 2, 1, 3).reshape(TOKENS, HEADS * DV)
    gated = (normed * jax.nn.sigmoid(output_gate_logit.astype(jnp.float32))).astype(jnp.bfloat16)
    mixed = block_sum(gated, projection, N_TP)
    mixed = mixed * lax.rsqrt(lax.optimization_barrier(jnp.mean(mixed * mixed, axis=-1, keepdims=True)) + EPSILON) * cell_output_gain
    first_sum = (residual.astype(jnp.float32) + mixed).astype(jnp.bfloat16)
    first_wide = lax.optimization_barrier(first_sum).astype(jnp.float32)
    normed_rows = (first_wide * lax.rsqrt(lax.optimization_barrier(jnp.mean(first_wide * first_wide, axis=-1, keepdims=True)) + EPSILON) * mixer_input_gain).astype(jnp.bfloat16)
    gate_value = jnp.dot(normed_rows, mixer_gate_weight, preferred_element_type=jnp.float32)
    up_value = jnp.dot(normed_rows, mixer_up_weight, preferred_element_type=jnp.float32)
    activated = (jax.nn.silu(gate_value) * up_value).astype(jnp.bfloat16)
    channel_out = block_sum(activated, mixer_down_weight, N_TP)
    return (first_wide + 0.5 * channel_out).astype(jnp.bfloat16)
```

```python
import functools

import jax
import jax.numpy as jnp
from jax import lax
from jax.sharding import PartitionSpec as P

DQK = 128
DV = 256
EPSILON = 1e-06
LOWEST_LOG = -1e30
STATE_PAD = 16


class Layout:
    def __init__(self, mesh):
        self.n_sp = mesh.shape["sp"]
        self.n_tp = mesh.shape["tp"]
        places = [getattr(d, "coords", None) for d in mesh.devices[:, 0]]
        self.inner = 1
        if places[0] is not None:
            while self.inner < self.n_sp and places[self.inner][2] == places[0][2]:
                self.inner += 1
            if self.n_sp % self.inner:
                self.inner = 1
        self.outer = self.n_sp // self.inner
        self.near = 2 if self.n_tp % 2 == 0 else 1
        self.far = self.n_tp // self.near

    def cycle(self):
        if self.inner == 1 or self.outer % 2:
            return list(range(self.n_sp))
        order = []
        for z in range(self.outer):
            row = list(range(1, self.inner))
            if z % 2:
                row.reverse()
            order += [z * self.inner + x for x in row]
        return order + [z * self.inner for z in reversed(range(self.outer))]

    def sp_inner(self, step):
        return [
            (z * self.inner + x, z * self.inner + (x + step) % self.inner)
            for z in range(self.outer)
            for x in range(self.inner)
        ]

    def sp_outer(self, step):
        return [
            (z * self.inner + x, (z + step) * self.inner + x)
            for z in range(self.outer - step)
            for x in range(self.inner)
        ]

    def tp_near(self, step=1):
        return [
            (y * self.near + c, y * self.near + (c + step) % self.near)
            for y in range(self.far)
            for c in range(self.near)
        ]

    def tp_far(self, step):
        return [
            (y * self.near + c, ((y + step) % self.far) * self.near + c)
            for y in range(self.far)
            for c in range(self.near)
        ]


def heads_first(array, heads, width):
    return array.reshape(array.shape[0], heads, width).transpose(1, 0, 2)


def dot(left, right, dims):
    return lax.dot_general(left, right, dims, preferred_element_type=jnp.float32)


class Ring:
    def __init__(self, layout, shard, split_axis):
        self.order = layout.cycle()
        n = len(self.order)
        self.n = n
        self.forward = [(self.order[i], self.order[(i + 1) % n]) for i in range(n)]
        self.backward = [(b, a) for a, b in self.forward]
        self.ahead = self.behind = shard
        self.shard = shard
        self.split_axis = split_axis
        self.step = 0
        self.pieces = [(0, 0, shard)]

    def hop(self):
        self.step += 1
        k = self.step
        if 2 * k < self.n:
            self.ahead = lax.ppermute(self.ahead, "sp", self.forward)
            self.behind = lax.ppermute(self.behind, "sp", self.backward)
            self.pieces += [(-k, 0, self.ahead), (k, 0, self.behind)]
        elif 2 * k == self.n:
            half = self.shard.shape[self.split_axis] // 2
            low = lax.slice_in_dim(self.ahead, 0, half, axis=self.split_axis)
            high = lax.slice_in_dim(self.behind, half, 2 * half, axis=self.split_axis)
            self.pieces += [
                (-k, 0, lax.ppermute(low, "sp", self.forward)),
                (k, half, lax.ppermute(high, "sp", self.backward)),
            ]

    def owner(self, offset):
        table = [0] * self.n
        for i, device in enumerate(self.order):
            table[device] = self.order[(i + offset) % self.n]
        return jnp.asarray(table, jnp.int32)[lax.axis_index("sp")]

    def whole(self, join_axis):
        shape = list(self.shard.shape)
        extent = shape[join_axis]
        shape[join_axis] *= self.n
        out = jnp.zeros(shape, self.shard.dtype)
        for offset, start, piece in self.pieces:
            at = [0] * len(shape)
            at[self.split_axis] = start
            at[join_axis] = at[join_axis] + self.owner(offset) * extent
            out = lax.dynamic_update_slice(out, piece, at)
        return out


def split_three(value):
    high = lax.reduce_precision(value, 8, 7)
    rest = value - high
    middle = lax.reduce_precision(rest, 8, 7)
    return [high, middle, rest - middle]


def pack_state(memory, normalizer, decay, peak):
    heads = memory.shape[0]
    scalars = jnp.stack(split_three(decay) + split_three(peak), axis=-1)
    scalars = jnp.pad(scalars, ((0, 0), (0, DQK - 6)))
    rows = jnp.concatenate(
        [normalizer[:, None], scalars[:, None], jnp.zeros((heads, STATE_PAD - 2, DQK), jnp.float32)],
        axis=1,
    )
    return jnp.concatenate([memory, rows], axis=1).astype(jnp.bfloat16)


def unpack_state(packed):
    wide = packed.astype(jnp.float32)
    scalars = wide[:, DV + 1]
    decay = scalars[:, 0] + (scalars[:, 1] + scalars[:, 2])
    peak = scalars[:, 3] + (scalars[:, 4] + scalars[:, 5])
    return wide[:, : DV + 1], decay, peak


def join_all(states):
    after = jnp.zeros_like(states[0][1])
    levels = []
    for state, decay, peak, present in reversed(states):
        levels.append(jnp.where(present, after + peak, LOWEST_LOG))
        after = after + jnp.where(present, decay, 0.0)
    levels.reverse()
    top = functools.reduce(jnp.maximum, levels)
    total = None
    for (state, _, _, present), level in zip(states, levels):
        scale = jnp.where(present, jnp.exp(level - top), 0.0)
        term = scale[:, None, None] * state
        total = term if total is None else total + term
    return total, after, top


def exchange_state(layout, memory, normalizer, decay, peak):
    mine = lax.axis_index("sp")
    z, x = mine // layout.inner, mine % layout.inner
    own = pack_state(memory, normalizer, decay, peak)
    by_shift = [own] + [
        lax.ppermute(own, "sp", layout.sp_inner(s)) for s in range(1, layout.inner)
    ]
    row = [unpack_state(p) for p in by_shift]

    def ordered(limit):
        out = []
        for position in range(layout.inner):
            shift = (x - position) % layout.inner
            pick = lambda i: functools.reduce(
                lambda acc, s: jnp.where(shift == s, row[s][i], acc),
                range(1, layout.inner),
                row[0][i],
            )
            out.append((pick(0), pick(1), pick(2), position < limit))
        return out

    full = join_all(ordered(layout.inner))
    whole_row = pack_state(full[0][:, :DV], full[0][:, DV], full[1], full[2])
    earlier = []
    for s in range(layout.outer - 1, 0, -1):
        got = unpack_state(lax.ppermute(whole_row, "sp", layout.sp_outer(s)))
        earlier.append((*got, z >= s))
    earlier += ordered(x)[: layout.inner - 1]
    if not earlier:
        zero = jnp.zeros_like(memory[:, :1, 0] * 0)
        return (jnp.zeros((memory.shape[0], DV + 1, DQK), jnp.float32), decay * 0, decay * 0 + LOWEST_LOG)
    return join_all(earlier)


def gather_near_far(layout, block):
    far = [block] + [lax.ppermute(block, "tp", layout.tp_far(s)) for s in range(1, layout.far)]
    if layout.near == 1:
        return far
    return [p for b in far for p in (b, lax.ppermute(b, "tp", layout.tp_near()))]


def scatter_sum(layout, partial):
    rows, width = partial.shape
    cols = width // layout.n_tp
    mine = lax.axis_index("tp")
    y, c = mine // layout.near, mine % layout.near
    blocks = partial.reshape(rows, layout.far, layout.near * cols)
    low = blocks.astype(jnp.bfloat16)
    kept = lax.dynamic_slice_in_dim(low, c * cols, cols, 2).astype(jnp.float32)
    if layout.near == 2:
        given = lax.dynamic_slice_in_dim(low, (1 - c) * cols, cols, 2)
        kept = kept + lax.ppermute(given, "tp", layout.tp_near()).astype(jnp.float32)
    total = lax.dynamic_slice_in_dim(kept, y, 1, 1)[:, 0]
    for s in range(1, layout.far):
        given = lax.dynamic_slice_in_dim(kept, (y + s) % layout.far, 1, 1)[:, 0]
        total = total + lax.ppermute(
            given.astype(jnp.bfloat16), "tp", layout.tp_far(s)
        ).astype(jnp.float32)
    return total


def body(
    layout,
    residual,
    query_matrix,
    key_matrix,
    value_matrix,
    output_gate_logit,
    input_gate_log,
    forget_gate_logit,
    extra_head_decay,
    head_norm_gain,
    projection,
    cell_output_gain,
    mixer_input_gain,
    mixer_gate_weight,
    mixer_up_weight,
    mixer_down_weight,
):
    length, width = residual.shape
    heads = input_gate_log.shape[1]
    gate_ring = Ring(layout, mixer_gate_weight, 0)
    up_ring = Ring(layout, mixer_up_weight, 0)
    down_ring = Ring(layout, mixer_down_weight, 0)
    for _ in range(layout.n_sp // 2):
        gate_ring.hop()
        up_ring.hop()
    for _ in range(layout.n_sp // 2):
        down_ring.hop()
    proj_blocks = gather_near_far(layout, projection)

    query = heads_first(query_matrix, heads, DQK)
    key = heads_first(key_matrix, heads, DQK)
    value = heads_first(value_matrix, heads, DV)
    in_logs = input_gate_log.T
    running_log = jnp.cumsum((jax.nn.log_sigmoid(forget_gate_logit) + extra_head_decay).T, axis=-1)
    last = running_log[:, -1]
    lifted = last[:, None] - running_log + in_logs
    peak = jnp.max(lifted, axis=-1)
    weights = jnp.exp(lifted - peak[:, None])
    weighted = (weights[:, :, None] * value.astype(jnp.float32)).astype(jnp.bfloat16)
    memory = dot(weighted, key, (((1,), (1,)), ((0,), (0,))))
    normalizer = dot(weights[:, None].astype(jnp.bfloat16), key, (((2,), (1,)), ((0,), (0,))))[:, 0]
    prior, prior_decay, prior_peak = exchange_state(layout, memory, normalizer, last, peak)

    start = jnp.maximum(prior_decay, prior_peak)
    prior = (jnp.exp(prior_peak - start)[:, None, None] * prior).astype(jnp.bfloat16)
    positions = lax.broadcasted_iota(jnp.int32, (length, length), 0)
    causal = positions >= lax.broadcasted_iota(jnp.int32, (length, length), 1)
    spread = running_log[:, :, None] - running_log[:, None, :] + in_logs[:, None, :]
    spread = jnp.where(causal[None], spread, -jnp.inf)
    carried = running_log + start[:, None]
    running = jnp.maximum(carried, jnp.max(spread, axis=-1))
    scores = dot(query, key, (((2,), (2,)), ((0,), (0,)))) * DQK ** (-0.5)
    inner = jnp.exp(spread - running[:, :, None]) * scores
    scaled = jnp.exp(carried - running) * DQK ** (-0.5)
    numerator = dot(inner.astype(jnp.bfloat16), value, (((2,), (1,)), ((0,), (0,))))
    crossed = dot(query, prior, (((2,), (2,)), ((0,), (0,))))
    numerator = numerator + scaled[:, :, None] * crossed[:, :, :DV]
    denominator = jnp.sum(inner, axis=-1) + scaled * crossed[:, :, DV]
    cells = numerator / jnp.maximum(jnp.abs(denominator), jnp.exp(-running))[:, :, None]

    centered = cells - jnp.mean(cells, axis=-1, keepdims=True)
    normed = centered * lax.rsqrt(jnp.mean(centered * centered, axis=-1, keepdims=True) + EPSILON)
    normed = normed * head_norm_gain.reshape(heads, DV)[:, None, :]
    normed = normed.transpose(1, 0, 2).reshape(length, heads * DV)
    gated = (normed * jax.nn.sigmoid(output_gate_logit.astype(jnp.float32))).astype(jnp.bfloat16)

    gated_blocks = gather_near_far(layout, gated)
    mixed = jnp.dot(
        jnp.concatenate(gated_blocks, axis=1),
        jnp.concatenate(proj_blocks, axis=0),
        preferred_element_type=jnp.float32,
    )
    squares = jnp.mean(mixed * mixed, axis=-1, keepdims=True)
    mixed = mixed * lax.rsqrt(squares + EPSILON) * cell_output_gain
    first_sum = (residual.astype(jnp.float32) + mixed).astype(jnp.bfloat16)
    first_wide = lax.optimization_barrier(first_sum).astype(jnp.float32)
    first_squares = jnp.mean(first_wide * first_wide, axis=-1, keepdims=True)
    normed_rows = (
        first_wide * lax.rsqrt(first_squares + EPSILON) * mixer_input_gain
    ).astype(jnp.bfloat16)

    gate_value = jnp.dot(normed_rows, gate_ring.whole(0), preferred_element_type=jnp.float32)
    up_value = jnp.dot(normed_rows, up_ring.whole(0), preferred_element_type=jnp.float32)
    activated = (jax.nn.silu(gate_value) * up_value).astype(jnp.bfloat16)
    down_terms = jnp.dot(activated, down_ring.whole(1), preferred_element_type=jnp.float32)
    channel_out = scatter_sum(layout, down_terms)
    cols = width // layout.n_tp
    own_first = lax.dynamic_slice_in_dim(first_wide, lax.axis_index("tp") * cols, cols, 1)
    return (own_first + 0.5 * channel_out).astype(jnp.bfloat16)


def solution(mesh):
    return jax.shard_map(
        functools.partial(body, Layout(mesh)),
        mesh=mesh,
        in_specs=(
            P("sp", None),
            P("sp", "tp"),
            P("sp", "tp"),
            P("sp", "tp"),
            P("sp", "tp"),
            P("sp", "tp"),
            P("sp", "tp"),
            P("sp", "tp"),
            P("tp"),
            P("tp", None),
            P(),
            P(),
            P("sp", "tp"),
            P("sp", "tp"),
            P("tp", "sp"),
        ),
        out_specs=P("sp", "tp"),
        check_vma=False,
    )
```
